512 devices in a mesh: ep: 32 (over z, core), tp: 16 (over y, x).
Axes of the slice: x: 4, y: 4, z: 16, core: 2. Of those that a mesh axis runs over, the one named last changes fastest.
Arguments:
- queries: bfloat16 [16384, 2048], P('ep', 'tp'), may hold values from -220 to 220
- keys: bfloat16 [16384, 2048], P('ep', 'tp'), may hold values from -6 to 6
- values: bfloat16 [16384, 2048], P('ep', 'tp'), may hold values from -6 to 6
- log_gate_sums: float32 [16384, 16], P(None, 'tp'), may hold values from -16384 to 0, as said below
- mixer_weight: bfloat16 [2048, 2048], P('tp'), may hold values from -2.5 to 2.5
- moe_rows: bfloat16 [6144, 2048], P('ep'), may hold values from -6 to 6
- route_ids: int32 [6144, 2], P('ep'), may hold values from 0 to 31, all different within a row; in each aligned block of 192 rows (0 to 191, 192 to 383, ...) at most 18 rows name the same one
- group_gate: float32 [6144], P('ep'), may hold values from 0.25 to 1
- inner_gate: float32 [6144, 2], P('ep'), may hold values from 0.2 to 1
- norm_gain: float32 [2048], replicated, may hold values from 0.1 to 1.9
- gate_weight: bfloat16 [32, 2048, 4096], P('ep', None, 'tp'), may hold values from -0.125 to 0.125
- up_weight: bfloat16 [32, 2048, 4096], P('ep', None, 'tp'), may hold values from -0.125 to 0.125
- down_weight: bfloat16 [32, 4096, 2048], P('ep', 'tp'), may hold values from -0.09375 to 0.09375
Outputs:
- mixer_out: bfloat16 [16384, 2048], P('ep', 'tp')
- moe_out: bfloat16 [6144, 2048], P('ep', 'tp')
The draws below stay inside these ranges and needn't reach their ends.
Inputs may be any that keep to these rules, and one draw needn't show every extreme that they name: `route_ids`: each row names 2 different experts; among the rows of one index of ep no expert is named more than 18 times, a bound that some block reaches. `log_gate_sums`: never rising along the positions of a head.
All inputs are finite; a program needn't handle non-finite values.
Results may differ from the reference program's by a relative error of at most 0.015.
Values may be sent and summed in bfloat16 or wider, within the bound.
A program may use at most 64 MiB of HBM per device.

```python
import math
import jax
import jax.numpy as jnp
import numpy as np
from jax import lax

D = 2048
HEAD_COUNT = 16
HEAD_DIM = 128
FF = 4096
TOPK = 2
RA = 512
RM = 192
EXPERTS = 32
CAP = 18
SEQUENCE_LENGTH = 16384
TOK_M = 6144
N_EP = 32
N_TP = 16


def draw_pair(base_key):
    mixed_key = jax.random.fold_in(base_key, 11)
    first_key, second_key = jax.random.split(mixed_key, 2)
    width_all = HEAD_COUNT * HEAD_DIM
    key_rows = jax.random.truncated_normal(first_key, -6.0, 6.0, (SEQUENCE_LENGTH, width_all), jnp.float32)
    query_rows = jax.random.truncated_normal(second_key, -6.0, 6.0, (SEQUENCE_LENGTH, width_all), jnp.float32)
    return (query_rows, key_rows)


def draw_queries(key, part):
    return draw_pair(key)[0].astype(jnp.bfloat16)


def draw_keys(key, part):
    return draw_pair(key)[1].astype(jnp.bfloat16)


def draw_log_gate_sums(key, part):
    mixed_key = jax.random.fold_in(key, 23)
    order_key, slow_key, fast_key, block_key, rough_key, location_key, depth_random_key = jax.random.split(mixed_key, 7)
    order = jax.random.permutation(order_key, HEAD_COUNT)
    slow_heads = order >= HEAD_COUNT // 2
    rough = jax.random.uniform(rough_key, (SEQUENCE_LENGTH, HEAD_COUNT), jnp.float32, 0.5, 1.5)
    slow_rate = jax.random.uniform(slow_key, (HEAD_COUNT,), jnp.float32, 0.3, 0.7) / SEQUENCE_LENGTH
    fast_rate = 1.0 / jax.random.uniform(fast_key, (HEAD_COUNT,), jnp.float32, 30.0, 100.0)
    head_rate = jnp.where(slow_heads, slow_rate, fast_rate)
    block_factor = jnp.exp(jax.random.uniform(block_key, (SEQUENCE_LENGTH // RA,), jnp.float32, -0.7, 0.7))
    position_factor = jnp.repeat(block_factor, RA)
    logarithm_steps = -head_rate[None, :] * position_factor[:, None] * rough
    surge_rows = jax.random.randint(location_key, (2,), 0, SEQUENCE_LENGTH)
    surge_depth = jnp.log(jax.random.uniform(depth_random_key, (2, HEAD_COUNT), jnp.float32, 0.5, 0.8))
    logarithm_steps = logarithm_steps.at[surge_rows].add(surge_depth)
    return jnp.cumsum(logarithm_steps, axis=0)


def shard_levels(key, dims, shards, smallest, largest):
    level = 1.0
    for dim, parts in shards:
        draws = jax.random.uniform(jax.random.fold_in(jax.random.fold_in(key, 6), dim), (parts,), jnp.float32, smallest / len(shards), largest / len(shards))
        level = level * jnp.repeat(jnp.exp(draws), dims[dim] // parts).reshape((-1,) + (1,) * (len(dims) - 1 - dim))
    return level


def assign_block(stream_key, own, number, rows, amount, top, reach, lean):
    ranking = jax.random.permutation(stream_key, amount)
    packed, common = portions_of(amount, rows * top, reach, lean, True), portions_of(amount, rows * top, reach, lean, False)
    places = jnp.arange(amount)

    def named(tallies, offset_by):
        used = int((tallies > 0).sum())
        fixed = max(1, used // 4)
        passed = fixed + (places - fixed + offset_by * (used - fixed)) % max(1, amount - fixed)
        return jnp.zeros((amount,), jnp.int32).at[ranking[jnp.where(places < fixed, places, passed)]].set(jnp.asarray(tallies, jnp.int32))

    tallies = jnp.where(number % 4 == 0, named(packed, number // 4), named(common, number - number // 4 - 1))
    mixed = jax.random.permutation(jax.random.fold_in(own, 3), amount)
    donor, receiver = mixed[0:amount // 2 * 2:2], mixed[1:amount // 2 * 2:2]
    room = jnp.minimum(tallies[donor] - 1, reach - tallies[receiver]) // 2
    room = jnp.where((donor == ranking[0]) | (receiver == ranking[0]) | (tallies[receiver] == 0), 0, jnp.maximum(room, 0))
    passed = jax.random.randint(jax.random.fold_in(own, 4), (amount // 2,), 0, 1 << 20) % (room + 1)
    tallies = tallies.at[donor].add(-passed).at[receiver].add(passed)
    items = jnp.searchsorted(jnp.cumsum(tallies), jnp.arange(rows * top), side="right").astype(jnp.int32)
    grid = items.reshape(top, rows).T
    grid = grid[jax.random.permutation(jax.random.fold_in(own, 1), rows)]
    offset_by = jax.random.randint(jax.random.fold_in(own, 2), (rows, 1), 0, top)
    return jnp.take_along_axis(grid, (jnp.arange(top)[None, :] + offset_by) % top, axis=1)


def portions_of(number_of, total, limit, lean, full):
    weights = [(1 << 20) // math.isqrt(standing ** lean) + 1 for standing in range(1, number_of + 1)]
    largest = limit if full else min(limit, max(-(-total // number_of), total * weights[0] // sum(weights)))
    least = 1 if total - largest >= number_of - 1 else 0
    holding, rest = [largest] + [least] * (number_of - 1), total - largest - least * (number_of - 1)
    while rest > 0:
        free = [i for i in range(1, number_of) if holding[i] < largest] or [i for i in range(1, number_of) if holding[i] < limit]
        mass, left = sum([weights[i] for i in free]), rest
        for i in free:
            addition = min(limit - holding[i], max(1, left * weights[i] // mass), rest)
            holding[i] = holding[i] + addition
            rest = rest - addition
    return np.array(holding)


def noise(own_key, extent, scale, most, cuts=(), kind=jnp.bfloat16):
    drawn = jax.random.normal(own_key, extent, jnp.float32) * scale
    if len(cuts) > 0:
        drawn = shard_levels(own_key, extent, cuts, -0.22, 0.18) * drawn
    return jnp.clip(drawn, min=-most, max=most).astype(kind)


def setup_inputs(seed: int = 0) -> dict:
    splits = jax.random.split(jax.random.key(seed), 14)
    queries = draw_queries(jax.random.fold_in(splits[13], 71), 0)
    keys = draw_keys(jax.random.fold_in(splits[13], 71), 0)
    values = noise(splits[2], (SEQUENCE_LENGTH, HEAD_COUNT * HEAD_DIM), 1.0, 6.0, ((0, 32), (1, 16)))
    log_gate_sums = draw_log_gate_sums(jax.random.fold_in(splits[13], 71), 0)
    mixer_weight = noise(splits[4], (HEAD_COUNT * HEAD_DIM, D), (8 * (HEAD_COUNT * HEAD_DIM) ** -0.5), 2.5, ((0, 16),))
    moe_rows = noise(splits[5], (TOK_M, D), 1.0, 6.0, ((0, 32),))
    route_ids_keys = jax.random.split(jax.random.fold_in(splits[6], 1), TOK_M // RM)
    route_ids_turns = jax.random.permutation(jax.random.fold_in(splits[6], 3), TOK_M // RM)
    route_ids = jax.vmap(lambda own, number: assign_block(jax.random.fold_in(splits[6], 2), own, number, RM, EXPERTS, TOPK, CAP, 2))(route_ids_keys, route_ids_turns).reshape((TOK_M, TOPK))
    group_gate = jnp.clip(jnp.exp(math.log(1.0) - 1.3862944 * jax.random.uniform(splits[7], (TOK_M,), jnp.float32) ** shard_levels(splits[7], (TOK_M,), ((0, 32),), -0.2, 0.2)), 0.25, 1.0)
    inner_gate = jnp.clip(jnp.exp(math.log(1.0) - 1.609438 * jax.random.uniform(splits[8], (TOK_M, TOPK), jnp.float32) ** shard_levels(splits[8], (TOK_M, TOPK), ((0, 32),), -0.2, 0.2)), 0.2, 1.0)
    norm_gain = jnp.clip(1.0 + 0.18 * jax.random.normal(splits[9], (D,), jnp.float32), 0.1, 1.9)
    gate_weight = noise(splits[10], (EXPERTS, D, FF), D ** -0.5, 0.125, ((0, 32), (2, 16)))
    up_weight = noise(splits[11], (EXPERTS, D, FF), D ** -0.5, 0.125, ((0, 32), (2, 16)))
    down_weight = noise(splits[12], (EXPERTS, FF, D), FF ** -0.5, 0.09375, ((0, 32), (1, 16)))
    return {"queries": queries, "keys": keys, "values": values, "log_gate_sums": log_gate_sums, "mixer_weight": mixer_weight, "moe_rows": moe_rows, "route_ids": route_ids, "group_gate": group_gate, "inner_gate": inner_gate, "norm_gain": norm_gain, "gate_weight": gate_weight, "up_weight": up_weight, "down_weight": down_weight}


LOW_SCORE = -1e+30
NORM_EPS = 1e-06

def attend_head(head_queries, head_keys, head_values, head_gates):
    inv_root = HEAD_DIM ** (-0.5)

    def query_block(block_index):
        row_offset = block_index * RA
        queries_here = lax.dynamic_slice_in_dim(head_queries, row_offset, RA, 0)
        query_gates = lax.dynamic_slice_in_dim(head_gates, row_offset, RA, 0)
        query_pos = row_offset + jnp.arange(RA, dtype=jnp.int32)

        def key_step(key_index, running):
            running_max, weight_sum, weighted = running
            key_offset = key_index * RA
            key_rows = lax.dynamic_slice_in_dim(head_keys, key_offset, RA, 0)
            value_rows = lax.dynamic_slice_in_dim(head_values, key_offset, RA, 0)
            key_gates = lax.dynamic_slice_in_dim(head_gates, key_offset, RA, 0)
            key_pos = key_offset + jnp.arange(RA, dtype=jnp.int32)
            scores = jnp.dot(queries_here, key_rows.T, preferred_element_type=jnp.float32) * inv_root
            scores = scores + query_gates[:, None] - key_gates[None, :]
            allowed = key_pos[None, :] <= query_pos[:, None]
            scores = jnp.where(allowed, scores, LOW_SCORE)
            new_max = jnp.maximum(running_max, lax.optimization_barrier(jnp.max(scores, axis=1)))
            shrink = jnp.exp(running_max - new_max)
            weights_now = jnp.where(allowed, jnp.exp(scores - new_max[:, None]), 0.0)
            weight_sum = weight_sum * shrink + lax.optimization_barrier(jnp.sum(weights_now, axis=1))
            weighted = weighted * shrink[:, None] + jnp.dot(weights_now.astype(jnp.bfloat16), value_rows, preferred_element_type=jnp.float32)
            return (new_max, weight_sum, weighted)
        start_state = (jnp.full((RA,), LOW_SCORE, jnp.float32), jnp.zeros((RA,), jnp.float32), jnp.zeros((RA, HEAD_DIM), jnp.float32))
        running_max, weight_sum, weighted = lax.fori_loop(0, block_index + 1, key_step, start_state)
        return (weighted / weight_sum[:, None]).astype(jnp.bfloat16)
    return lax.map(query_block, jnp.arange(N_EP, dtype=jnp.int32)).reshape(SEQUENCE_LENGTH, HEAD_DIM)

def attend_group(grouped):
    return attend_head(grouped[0], grouped[1], grouped[2], grouped[3])

def reference(queries, keys, values, log_gate_sums, mixer_weight, moe_rows, route_ids, group_gate, inner_gate, norm_gain, gate_weight, up_weight, down_weight):
    head_split = (SEQUENCE_LENGTH, HEAD_COUNT, HEAD_DIM)
    per_head = (queries.reshape(head_split).transpose(1, 0, 2), keys.reshape(head_split).transpose(1, 0, 2), values.reshape(head_split).transpose(1, 0, 2), log_gate_sums.T)
    attended = lax.map(attend_group, per_head)
    attended = attended.transpose(1, 0, 2).reshape(SEQUENCE_LENGTH, HEAD_COUNT * HEAD_DIM)
    head_cols = HEAD_COUNT * HEAD_DIM // N_TP
    mixer_total = jnp.zeros((SEQUENCE_LENGTH, D), jnp.float32)
    for group_index in range(N_TP):
        col_start = group_index * head_cols
        partial_value = jnp.dot(attended[:, col_start:col_start + head_cols], mixer_weight[col_start:col_start + head_cols], preferred_element_type=jnp.float32).astype(jnp.bfloat16)
        partial_value = lax.optimization_barrier(partial_value)
        mixer_total = mixer_total + partial_value.astype(jnp.float32)
    mixer_out = mixer_total.astype(jnp.bfloat16)
    rows_float = moe_rows.astype(jnp.float32)
    normed = (rows_float * lax.rsqrt(lax.optimization_barrier(jnp.mean(rows_float * rows_float, axis=1, keepdims=True)) + NORM_EPS) * norm_gain).astype(jnp.bfloat16)
    route_weight = group_gate[:, None] * inner_gate / lax.optimization_barrier(jnp.sum(inner_gate, axis=1, keepdims=True))
    onehot = (route_ids[:, :, None] == jnp.arange(EXPERTS, dtype=jnp.int32)[None, None, :]).astype(jnp.int32)
    onehot = onehot.reshape(N_EP, RM * TOPK, EXPERTS)
    earlier_hits = jnp.cumsum(onehot, axis=1) - onehot
    rank_here = lax.optimization_barrier(jnp.sum(earlier_hits * onehot, axis=2)).reshape(TOK_M, TOPK)
    source_block = (jnp.arange(TOK_M, dtype=jnp.int32) // RM)[:, None]
    slot_column = (source_block * CAP + rank_here).astype(jnp.int32)
    token_ids = jnp.broadcast_to(jnp.arange(TOK_M, dtype=jnp.int32)[:, None], (TOK_M, TOPK))
    slot_table = jnp.zeros((EXPERTS, N_EP * CAP), jnp.int32).at[route_ids, slot_column].set(token_ids)
    hidden_cols = FF // N_TP

    def run_expert(expert_index):
        expert_rows = normed[slot_table[expert_index]]
        gate_act = jnp.dot(expert_rows, gate_weight[expert_index], preferred_element_type=jnp.float32)
        up_act = jnp.dot(expert_rows, up_weight[expert_index], preferred_element_type=jnp.float32)
        hidden = (jax.nn.silu(gate_act) * up_act).astype(jnp.bfloat16)
        expert_total = jnp.zeros((N_EP * CAP, D), jnp.float32)
        for group_index in range(N_TP):
            col_start = group_index * hidden_cols
            expert_part = jnp.dot(hidden[:, col_start:col_start + hidden_cols], down_weight[expert_index, col_start:col_start + hidden_cols], preferred_element_type=jnp.float32).astype(jnp.bfloat16)
            expert_part = lax.optimization_barrier(expert_part)
            expert_total = expert_total + expert_part.astype(jnp.float32)
        return expert_total.astype(jnp.bfloat16)
    expert_out = lax.map(run_expert, jnp.arange(EXPERTS, dtype=jnp.int32))
    picked = expert_out[route_ids, slot_column].astype(jnp.float32)
    moe_out = lax.optimization_barrier(jnp.sum(route_weight[:, :, None] * picked, axis=1)).astype(jnp.bfloat16)
    return (mixer_out, moe_out)
```

```python
import functools

import jax
import jax.numpy as jnp
from jax import lax
from jax.experimental import pallas as pl
from jax.experimental.pallas import tpu as pltpu
from jax.sharding import PartitionSpec as P

LOW_SCORE = -1e30
NORM_EPS = 1e-06
LOG2E = 1.4426950408889634
LANES = 128
MESH = pl.DeviceIdType.MESH
F32 = jnp.float32
BF16 = jnp.bfloat16


def one_hot(mask):
    return jnp.where(mask, 1.0, 0.0).astype(BF16)


class Links:

    def __init__(self, sems, limit):
        self.sems, self.limit, self.used, self.sent = sems, limit, 0, []

    def new(self):
        self.used += 1
        assert self.used <= self.limit
        return self.sems.at[self.used - 1]

    def copy(self, src, dst, device):
        c = pltpu.make_async_remote_copy(
            src_ref=src,
            dst_ref=dst,
            send_sem=self.new(),
            recv_sem=self.new(),
            device_id=device,
            device_id_type=MESH,
        )
        return c

    def start(self, c):
        c.start()
        self.sent.append(c)

    def finish(self):
        for c in self.sent:
            c.wait_send()
        self.sent = []


class GatherLine:

    def __init__(self, links, n, c, dev, block, first, second):
        self.links, self.n = links, n
        nxt, prv = (c + 1) % n, (c + n - 1) % n
        if n == 1:
            return
        self.up = links.copy(block(c), block(c), dev(nxt))
        if n == 4:
            self.down = links.copy(block(c), block(c), dev(prv))
            self.relay_up = links.copy(first(block(prv)), first(block(prv)), dev(nxt))
            self.relay_down = links.copy(second(block(nxt)), second(block(nxt)), dev(prv))

    def begin(self):
        if self.n > 1:
            self.links.start(self.up)
        if self.n == 4:
            self.links.start(self.down)

    def relay(self):
        if self.n == 4:
            self.up.wait_recv()
            self.links.start(self.relay_up)
            self.down.wait_recv()
            self.links.start(self.relay_down)

    def end(self):
        if self.n == 2:
            self.up.wait_recv()
        if self.n == 4:
            self.relay_up.wait_recv()
            self.relay_down.wait_recv()


class SumLine:

    def __init__(self, links, n, c, dev, block, first, second, half_a, half_b, full_a, full_b):
        self.links, self.n, self.c, self.block = links, n, c, block
        self.first, self.second = first, second
        self.half_a, self.half_b, self.full_a, self.full_b = half_a, half_b, full_a, full_b
        nxt, prv, far = (c + 1) % n, (c + n - 1) % n, (c + 2) % n
        self.nxt, self.prv = nxt, prv
        if n == 1:
            return
        if n == 4:
            self.far_up = links.copy(first(block(far)), half_a, dev(nxt))
            self.far_down = links.copy(second(block(far)), half_b, dev(prv))
            self.down = links.copy(block(prv), full_b, dev(prv))
        self.up = links.copy(block(nxt), full_a, dev(nxt))

    def begin(self):
        if self.n == 4:
            self.links.start(self.far_up)
            self.links.start(self.far_down)

    def relay(self):
        if self.n == 4:
            self.far_up.wait_recv()
            part = self.first(self.block(self.nxt))
            part[...] = (part[...].astype(F32) + self.half_a[...].astype(F32)).astype(BF16)
            self.links.start(self.up)
            self.far_down.wait_recv()
            part = self.second(self.block(self.prv))
            part[...] = (part[...].astype(F32) + self.half_b[...].astype(F32)).astype(BF16)
            self.links.start(self.down)
        elif self.n == 2:
            self.links.start(self.up)

    def end(self):
        total = self.block(self.c)[...].astype(F32)
        if self.n > 1:
            self.up.wait_recv()
            total = total + self.full_a[...].astype(F32)
        if self.n == 4:
            self.down.wait_recv()
            total = total + self.full_b[...].astype(F32)
        return total


class SumPlane:

    def __init__(self, links, nx, ny, x, y, at_x, at_y, part, bufs):
        rows = part.shape[2]
        h = rows // 2
        q = h // 2
        (ha, hb, fa, fb, sa, ga, gb, ea, eb) = bufs[:9]
        (hc, hd, fc, fd, sb, gc, gd, ec, ed) = bufs[9:]
        self.sa, self.sb = sa, sb

        def wide_first(r):
            return r.at[:, pl.ds(0, q), :]

        def wide_second(r):
            return r.at[:, pl.ds(q, q), :]

        def flat_first(r):
            return r.at[pl.ds(0, q), :]

        def flat_second(r):
            return r.at[pl.ds(q, q), :]

        self.a1 = SumLine(
            links, nx, x, at_x, lambda c: part.at[:, c, pl.ds(0, h), :], wide_first, wide_second, ha, hb, fa, fb
        )
        self.b1 = SumLine(
            links, ny, y, at_y, lambda c: part.at[c, :, pl.ds(h, h), :], wide_first, wide_second, hc, hd, fc, fd
        )
        self.a2 = SumLine(links, ny, y, at_y, lambda c: sa.at[c], flat_first, flat_second, ga, gb, ea, eb)
        self.b2 = SumLine(links, nx, x, at_x, lambda c: sb.at[c], flat_first, flat_second, gc, gd, ec, ed)

    def steps(self, done):
        def begin():
            self.a1.begin()
            self.b1.begin()

        def relay():
            self.a1.relay()
            self.b1.relay()

        def turn():
            self.sa[...] = self.a1.end().astype(BF16)
            self.a2.begin()
            self.sb[...] = self.b1.end().astype(BF16)
            self.b2.begin()

        def relay2():
            self.a2.relay()
            self.b2.relay()

        def end():
            done(self.a2.end(), self.b2.end())

        return [begin, relay, turn, relay2, end]


def sum_buffers(nx, ny, rows):
    h = rows // 2
    q = h // 2

    def v(*shape):
        return pltpu.VMEM((*shape, LANES), BF16)

    return [
        v(ny, q), v(ny, q), v(ny, h), v(ny, h), v(ny, h), v(q), v(q), v(h), v(h),
        v(nx, q), v(nx, q), v(nx, h), v(nx, h), v(nx, h), v(q), v(q), v(h), v(h),
    ]


SEM_LIMIT = 240


def kernel(cfg, *refs):
    (nz, nx, ny, cap, slots, moe_at) = cfg
    (q_h, k_h, v_h, gates_h, mixw_h, rows_h, rids, rids_t, weight, gain, wg_h, wu_h, wd_h) = refs[:13]
    (out_mix, out_moe) = refs[13:15]
    (
        k_all, v_all, q_v, gk, acc, top,
        mixw, mix_part, att,
        rows_v, wg, wu, wd,
        disp, arrived, feats, part, back, ret,
        sems, dsem_s, dsem_r, rsem_s, rsem_r, lsem,
    ) = refs[15:40]
    mix_bufs = refs[40:58]
    moe_bufs = refs[58:76]

    ep_n, tp_n = 2 * nz, nx * ny
    ep, tp = lax.axis_index("ep"), lax.axis_index("tp")
    z, core = ep // 2, ep % 2
    y, x = tp // nx, tp % nx
    rows_a = q_h.shape[0]
    rows_m = rows_h.shape[0]
    width = rows_h.shape[1]
    experts = ep_n
    held = experts * cap
    links = Links(sems, SEM_LIMIT)

    def at_ep(p):
        return {"ep": p}

    def at_x(c):
        return {"tp": y * nx + c}

    def at_y(c):
        return {"tp": c * nx + x}

    own_rows = pl.ds(pl.multiple_of(core * rows_a, rows_a), rows_a)

    def mine(buf, chip):
        return buf.at[chip, own_rows, :]

    loads = [
        pltpu.make_async_copy(src, dst, lsem.at[i])
        for i, (src, dst) in enumerate(
            [
                (rows_h, rows_v),
                (k_h, mine(k_all, z)),
                (v_h, mine(v_all, z)),
                (q_h, q_v),
                (gates_h, gk),
                (wg_h, wg),
                (wu_h, wu),
                (wd_h, wd),
                (mixw_h, mixw),
            ]
        )
    ]
    for c in loads:
        c.start()

    barrier = pltpu.get_barrier_semaphore()

    def greet(o, carry):
        pl.semaphore_signal(barrier, inc=1, device_id=at_ep((ep + o) % ep_n), device_id_type=MESH)
        return carry

    lax.fori_loop(1, ep_n, greet, 0)
    for o in range(1, nx):
        pl.semaphore_signal(barrier, inc=1, device_id=at_x((x + o) % nx), device_id_type=MESH)
    for o in range(1, ny):
        pl.semaphore_signal(barrier, inc=1, device_id=at_y((y + o) % ny), device_id_type=MESH)

    loads[0].wait()
    ids_t = rids_t[...].astype(F32)
    expert_rows = lax.broadcasted_iota(jnp.int32, (experts, rows_m), 0).astype(F32)
    hit0, hit1 = ids_t[0:1] == expert_rows, ids_t[1:2] == expert_rows
    before = one_hot(
        lax.broadcasted_iota(jnp.int32, (rows_m, rows_m), 0)
        < lax.broadcasted_iota(jnp.int32, (rows_m, rows_m), 1)
    )
    rank = jnp.dot(one_hot(hit0 | hit1), before, preferred_element_type=F32)
    slot0 = ids_t[0:1] * slots + jnp.sum(jnp.where(hit0, rank, 0.0), axis=0, keepdims=True)
    slot1 = ids_t[1:2] * slots + jnp.sum(jnp.where(hit1, rank, 0.0), axis=0, keepdims=True)
    slot_rows = lax.broadcasted_iota(jnp.int32, (experts * slots, rows_m), 0).astype(F32)
    select = one_hot((slot_rows == slot0) | (slot_rows == slot1))
    squares = jnp.zeros((rows_m, LANES), F32)
    for b in range(width // LANES):
        r = rows_v[:, b * LANES : (b + 1) * LANES].astype(F32)
        squares = squares + r * r
    mean = jnp.sum(squares, axis=1, keepdims=True) / width
    own_cols = pl.ds(pl.multiple_of(tp * LANES, LANES), LANES)
    normed = (rows_v[:, own_cols].astype(F32) * lax.rsqrt(mean + NORM_EPS) * gain[:, own_cols]).astype(BF16)
    disp[...] = (
        jnp.dot(select, normed, preferred_element_type=F32).astype(BF16).reshape(experts, slots, LANES)
    )

    loads[1].wait()
    loads[2].wait()
    pl.semaphore_wait(barrier, ep_n - 1 + nx - 1 + ny - 1)

    def dispatch_copy(o):
        peer = (ep + o) % ep_n
        return pltpu.make_async_remote_copy(
            src_ref=disp.at[peer],
            dst_ref=arrived.at[ep],
            send_sem=dsem_s.at[o],
            recv_sem=dsem_r.at[o],
            device_id=at_ep(peer),
            device_id_type=MESH,
        )

    def return_copy(o):
        peer = (ep + o) % ep_n
        return pltpu.make_async_remote_copy(
            src_ref=back.at[peer],
            dst_ref=ret.at[ep],
            send_sem=rsem_s.at[o],
            recv_sem=rsem_r.at[o],
            device_id=at_ep(peer),
            device_id_type=MESH,
        )

    def each_peer(do):
        def step(o, carry):
            do(o)
            return carry

        lax.fori_loop(1, ep_n, step, 0)

    each_peer(lambda o: dispatch_copy(o).start())

    up_chip = at_ep(((z + 1) % nz) * 2 + core)
    down_chip = at_ep(((z + nz - 1) % nz) * 2 + core)
    partner = at_ep(z * 2 + 1 - core)
    half = nz // 2
    reach = {"k_up": half, "k_down": half - 1, "v_up": half - 1, "v_down": half}
    ring, cross = {}, {}
    for kind in ("k", "v"):
        buf = k_all if kind == "k" else v_all
        cross[kind, 0] = links.copy(mine(buf, z), mine(buf, z), partner)
        for way, sign, dev in (("up", -1, up_chip), ("down", 1, down_chip)):
            for d in range(1, reach[kind + "_" + way] + 1):
                sent = (z + sign * (d - 1) + nz) % nz
                got = (z + sign * d + nz) % nz
                ring[kind, way, d] = links.copy(mine(buf, sent), mine(buf, sent), dev)
                cross[kind, way, d] = links.copy(mine(buf, got), mine(buf, got), partner)

    for kind in ("k", "v"):
        for way in ("up", "down"):
            if (kind, way, 1) in ring:
                links.start(ring[kind, way, 1])
        links.start(cross[kind, 0])

    arrived[ep] = disp[ep]

    scale = LOG2E * LANES**-0.5
    chunk = 2 * rows_a
    q_block = min(256, rows_a)
    top[...] = jnp.full(top.shape, LOW_SCORE, F32)
    acc[...] = jnp.zeros(acc.shape, F32)
    loads[3].wait()
    loads[4].wait()
    base = jnp.max(gk[pl.ds(z, 1), own_rows], axis=1, keepdims=True)

    def attend(chip, masked):
        bias = (gk[pl.ds(chip, 1), :] - base) * LOG2E
        ones = jnp.ones((chunk, LANES), BF16)
        for i in range(rows_a // q_block):
            here = pl.ds(i * q_block, q_block)
            scores = (
                lax.dot_general(
                    q_v[here, :], k_all[chip], (((1,), (1,)), ((), ())), preferred_element_type=F32
                )
                * scale
                - bias
            )
            if masked:
                key_pos = lax.broadcasted_iota(jnp.int32, (q_block, chunk), 1)
                query_pos = lax.broadcasted_iota(jnp.int32, (q_block, chunk), 0) + core * rows_a + i * q_block
                scores = jnp.where(key_pos <= query_pos, scores, LOW_SCORE)
            old = top[here, :]
            new = jnp.maximum(old, jnp.max(scores, axis=1, keepdims=True))
            top[here, :] = new
            shrink = jnp.exp2(old - new)
            weights = jnp.exp2(scores - new[:, 0:1]).astype(BF16)
            both = jnp.concatenate([v_all[chip], ones], axis=1)
            add = jnp.dot(weights, both, preferred_element_type=F32)
            acc[here, :] = acc[here, :] * jnp.concatenate([shrink, shrink], axis=1) + add

    gather = {}
    h, qtr = held // 2, held // 4
    gather["a1"] = GatherLine(
        links, nx, x, at_x, lambda c: feats.at[y, c, pl.ds(0, h), :],
        lambda r: r.at[pl.ds(0, qtr), :], lambda r: r.at[pl.ds(qtr, qtr), :],
    )
    gather["b1"] = GatherLine(
        links, ny, y, at_y, lambda c: feats.at[c, x, pl.ds(h, h), :],
        lambda r: r.at[pl.ds(0, qtr), :], lambda r: r.at[pl.ds(qtr, qtr), :],
    )
    gather["a2"] = GatherLine(
        links, ny, y, at_y, lambda c: feats.at[c, :, pl.ds(0, h), :],
        lambda r: r.at[:, pl.ds(0, qtr), :], lambda r: r.at[:, pl.ds(qtr, qtr), :],
    )
    gather["b2"] = GatherLine(
        links, nx, x, at_x, lambda c: feats.at[:, c, pl.ds(h, h), :],
        lambda r: r.at[:, pl.ds(0, qtr), :], lambda r: r.at[:, pl.ds(qtr, qtr), :],
    )

    def packed_row(shape, dim):
        i = lax.broadcasted_iota(jnp.int32, shape, dim)
        return (i // cap) * slots + i % cap

    def moe_arrive():
        each_peer(lambda o: dispatch_copy(o).wait_recv())
        where_from = packed_row((held, 1), 0)
        pick = one_hot(where_from == lax.broadcasted_iota(jnp.int32, (held, experts * slots), 1))
        feats[y, x] = jnp.dot(
            pick, arrived[...].reshape(experts * slots, LANES), preferred_element_type=F32
        ).astype(BF16)
        gather["a1"].begin()
        gather["b1"].begin()

    def moe_gather_relay():
        gather["a1"].relay()
        gather["b1"].relay()

    def moe_gather_turn():
        gather["a1"].end()
        gather["a2"].begin()
        gather["b1"].end()
        gather["b2"].begin()

    def moe_gather_relay2():
        gather["a2"].relay()
        gather["b2"].relay()

    made = {}

    def moe_hidden():
        gather["a2"].end()
        gather["b2"].end()
        loads[5].wait()
        loads[6].wait()
        gate, up = 0.0, 0.0
        for yy in range(ny):
            block = jnp.concatenate([feats[yy, xx] for xx in range(nx)], axis=1)
            cols = slice(yy * nx * LANES, (yy + 1) * nx * LANES)
            gate = gate + jnp.dot(block, wg[cols, :], preferred_element_type=F32)
            up = up + jnp.dot(block, wu[cols, :], preferred_element_type=F32)
        made["hidden"] = (gate / (1.0 + jnp.exp(-gate)) * up).astype(BF16)

    def project(rows, weights_ref, dest):
        for b in range(0, tp_n, 2):
            both = jnp.dot(rows, weights_ref[:, b * LANES : (b + 2) * LANES], preferred_element_type=F32)
            for e in (0, 1):
                dest[(b + e) // nx, (b + e) % nx] = both[:, e * LANES : (e + 1) * LANES].astype(BF16)

    def expert_done(first, second):
        packed = jnp.concatenate([first, second], axis=0).astype(BF16)
        where_to = packed_row((1, held), 1)
        spread = one_hot(lax.broadcasted_iota(jnp.int32, (experts * slots, held), 0) == where_to)
        back[...] = (
            jnp.dot(spread, packed, preferred_element_type=F32).astype(BF16).reshape(experts, slots, LANES)
        )
        each_peer(lambda o: return_copy(o).start())
        ret[ep] = back[ep]

    expert_sum = SumPlane(links, nx, ny, x, y, at_x, at_y, part, moe_bufs).steps(expert_done)

    def moe_down():
        loads[7].wait()
        project(made["hidden"], wd, part)
        expert_sum[0]()

    def moe_combine():
        each_peer(lambda o: return_copy(o).wait_recv())
        ids = rids[...].astype(F32)
        expert_cols = lax.broadcasted_iota(jnp.int32, (rows_m, experts), 1).astype(F32)
        hits = [ids[:, k : k + 1] == expert_cols for k in (0, 1)]
        after = one_hot(
            lax.broadcasted_iota(jnp.int32, (rows_m, rows_m), 0)
            > lax.broadcasted_iota(jnp.int32, (rows_m, rows_m), 1)
        )
        ranks = jnp.dot(after, one_hot(hits[0] | hits[1]), preferred_element_type=F32)
        slot_cols = lax.broadcasted_iota(jnp.int32, (rows_m, experts * slots), 1).astype(F32)
        rows = ret[...].reshape(experts * slots, LANES)
        total = 0.0
        for k in (0, 1):
            slot = ids[:, k : k + 1] * slots + jnp.sum(jnp.where(hits[k], ranks, 0.0), axis=1, keepdims=True)
            picked = jnp.dot(one_hot(slot_cols == slot), rows, preferred_element_type=F32)
            total = total + weight[:, k : k + 1] * picked
        out_moe[...] = total.astype(BF16)

    moe = [
        moe_arrive,
        moe_gather_relay,
        moe_gather_turn,
        moe_gather_relay2,
        lambda: (moe_hidden(), moe_down()),
        expert_sum[1],
        expert_sum[2],
        expert_sum[3],
        expert_sum[4],
        moe_combine,
    ]

    def moe_slot(number):
        while moe_at and moe and moe_at[0] <= number:
            moe_at.pop(0)
            moe.pop(0)()

    moe_at = list(moe_at)

    cross["k", 0].wait_recv()
    cross["v", 0].wait_recv()
    attend(z, True)

    def pass_on(kind, d):
        for way in ("up", "down"):
            if (kind, way, d) in ring:
                ring[kind, way, d].wait_recv()
                if (kind, way, d + 1) in ring:
                    links.start(ring[kind, way, d + 1])
                links.start(cross[kind, way, d])

    def landed(d):
        for kind in ("k", "v"):
            for way in ("up", "down"):
                if (kind, way, d) in ring:
                    cross[kind, way, d].wait_recv()

    def attend_up(d):
        @pl.when(z >= d)
        def _():
            attend(z - d, False)

    def attend_down(d):
        @pl.when(z + d >= nz)
        def _():
            attend(z + d - nz, False)

    for d in range(1, half + 1):
        pass_on("k", d)
        if d > 1:
            landed(d - 1)
            attend_up(d - 1)
        moe_slot(2 * d - 1)
        pass_on("v", d)
        if d > 1:
            attend_down(d - 1)
        moe_slot(2 * d)
    landed(half)
    attend_up(half)

    @pl.when(z < half)
    def _():
        pass

    att[...] = (acc[:, 0:LANES] / acc[:, LANES:]).astype(BF16)

    def mix_done(first, second):
        out_mix[pl.ds(0, rows_a // 2), :] = first.astype(BF16)
        out_mix[pl.ds(rows_a // 2, rows_a // 2), :] = second.astype(BF16)

    mix = SumPlane(links, nx, ny, x, y, at_x, at_y, mix_part, mix_bufs).steps(mix_done)
    loads[8].wait()
    project(att[...], mixw, mix_part)
    mix.pop(0)()
    while mix or moe:
        if moe:
            moe.pop(0)()
        if mix:
            mix.pop(0)()
    links.finish()
    each_peer(lambda o: dispatch_copy(o).wait_send())
    each_peer(lambda o: return_copy(o).wait_send())


def body(sizes, moe_at, queries, keys, values, log_gate_sums, mixer_weight, moe_rows, route_ids,
         group_gate, inner_gate, norm_gain, gate_weight, up_weight, down_weight):
    nz, nx, ny = sizes
    rows_a, rows_m, width = queries.shape[0], moe_rows.shape[0], moe_rows.shape[1]
    experts = 2 * nz
    cap = 3 * rows_m * route_ids.shape[1] // (2 * experts)
    slots = -(-cap // 16) * 16
    hidden = gate_weight.shape[2]
    held = experts * cap
    route_weight = group_gate[:, None] * inner_gate / jnp.sum(inner_gate, axis=1, keepdims=True)
    gates = log_gate_sums.reshape(nz, 2 * rows_a)

    def v(*shape, dtype=BF16):
        return pltpu.VMEM(shape, dtype)

    scratch = [
        v(nz, 2 * rows_a, LANES), v(nz, 2 * rows_a, LANES), v(rows_a, LANES), v(nz, 2 * rows_a, dtype=F32),
        v(rows_a, 2 * LANES, dtype=F32), v(rows_a, LANES, dtype=F32),
        v(LANES, width), v(ny, nx, rows_a, LANES), v(rows_a, LANES),
        v(rows_m, width), v(width, hidden), v(width, hidden), v(hidden, width),
        v(experts, slots, LANES), v(experts, slots, LANES), v(ny, nx, held, LANES), v(ny, nx, held, LANES),
        v(experts, slots, LANES), v(experts, slots, LANES),
        pltpu.SemaphoreType.DMA((SEM_LIMIT,)),
        pltpu.SemaphoreType.DMA((2 * nz,)), pltpu.SemaphoreType.DMA((2 * nz,)),
        pltpu.SemaphoreType.DMA((2 * nz,)), pltpu.SemaphoreType.DMA((2 * nz,)),
        pltpu.SemaphoreType.DMA((9,)),
        *sum_buffers(nx, ny, rows_a),
        *sum_buffers(nx, ny, held),
    ]
    hbm = pl.BlockSpec(memory_space=pl.ANY)
    vm = pl.BlockSpec(memory_space=pltpu.VMEM)
    return pl.pallas_call(
        functools.partial(kernel, (nz, nx, ny, cap, slots, moe_at)),
        out_shape=(
            jax.ShapeDtypeStruct((rows_a, LANES), BF16),
            jax.ShapeDtypeStruct((rows_m, LANES), BF16),
        ),
        in_specs=[hbm] * 6 + [vm] * 4 + [hbm] * 3,
        out_specs=(vm, vm),
        scratch_shapes=scratch,
        compiler_params=pltpu.CompilerParams(
            collective_id=0, has_side_effects=True, vmem_limit_bytes=60 * 1024 * 1024
        ),
        name="step",
    )(
        queries, keys, values, gates, mixer_weight, moe_rows, route_ids, route_ids.T, route_weight,
        norm_gain.reshape(1, -1), gate_weight[0], up_weight[0], down_weight[0],
    )


MOE_AT = (5, 6, 7, 9, 11, 14, 16)


def plane_of(tp):
    side = 1
    while side * side < tp:
        side *= 2
    return side, tp // side


def solution(mesh, plane=None, moe_at=MOE_AT):
    nx, ny = plane or plane_of(mesh.shape["tp"])
    sizes = (mesh.shape["ep"] // 2, nx, ny)
    return jax.shard_map(
        functools.partial(body, sizes, moe_at),
        mesh=mesh,
        in_specs=(
            P("ep", "tp"),
            P("ep", "tp"),
            P("ep", "tp"),
            P(None, "tp"),
            P("tp", None),
            P("ep", None),
            P("ep", None),
            P("ep"),
            P("ep", None),
            P(),
            P("ep", None, "tp"),
            P("ep", None, "tp"),
            P("ep", "tp", None),
        ),
        out_specs=(P("ep", "tp"), P("ep", "tp")),
        check_vma=False,
    )
```

```python
import functools

import jax
import jax.numpy as jnp
from jax import lax
from jax.experimental import pallas as pl
from jax.experimental.pallas import tpu as pltpu
from jax.sharding import PartitionSpec as P

LOW_SCORE = -1e30
NORM_EPS = 1e-06
LOG2E = 1.4426950408889634
LANES = 128
MESH = pl.DeviceIdType.MESH
F32 = jnp.float32
BF16 = jnp.bfloat16


def one_hot(mask):
    return jnp.where(mask, 1.0, 0.0).astype(BF16)


class Links:

    def __init__(self, sems, limit):
        self.sems, self.limit, self.used, self.sent = sems, limit, 0, []

    def new(self):
        self.used += 1
        assert self.used <= self.limit
        return self.sems.at[self.used - 1]

    def copy(self, src, dst, device):
        c = pltpu.make_async_remote_copy(
            src_ref=src,
            dst_ref=dst,
            send_sem=self.new(),
            recv_sem=self.new(),
            device_id=device,
            device_id_type=MESH,
        )
        return c

    def start(self, c):
        c.start()
        self.sent.append(c)

    def finish(self):
        for c in self.sent:
            c.wait_send()
        self.sent = []


class GatherLine:

    def __init__(self, links, n, c, dev, block, first, second):
        self.links, self.n = links, n
        nxt, prv = (c + 1) % n, (c + n - 1) % n
        if n == 1:
            return

        def same(ref, to):
            return links.copy(ref, ref, dev(to))

        self.up = [same(first(block(c)), nxt), same(second(block(c)), nxt)]
        self.down = []
        if n == 4:
            self.down = [same(second(block(c)), prv), same(first(block(c)), prv)]
            self.relay_up = same(first(block(prv)), nxt)
            self.relay_down = same(second(block(nxt)), prv)

    def begin(self):
        if self.n == 1:
            return
        for k in (0, 1):
            self.links.start(self.up[k])
            if self.n == 4:
                self.links.start(self.down[k])

    def relay(self):
        if self.n == 4:
            self.up[0].wait_recv()
            self.links.start(self.relay_up)
            self.down[0].wait_recv()
            self.links.start(self.relay_down)

    def end(self):
        if self.n == 2:
            self.up[0].wait_recv()
            self.up[1].wait_recv()
        if self.n == 4:
            self.up[1].wait_recv()
            self.down[1].wait_recv()
            self.relay_up.wait_recv()
            self.relay_down.wait_recv()


class SumLine:

    def __init__(self, links, n, c, dev, block, first, second, half_a, half_b, full_a, full_b):
        self.links, self.n, self.c, self.block = links, n, c, block
        self.first, self.second = first, second
        self.half_a, self.half_b, self.full_a, self.full_b = half_a, half_b, full_a, full_b
        nxt, prv, far = (c + 1) % n, (c + n - 1) % n, (c + 2) % n
        self.nxt, self.prv = nxt, prv
        if n == 1:
            return
        if n == 4:
            self.far_up = links.copy(first(block(far)), half_a, dev(nxt))
            self.far_down = links.copy(second(block(far)), half_b, dev(prv))
            self.down_plain = links.copy(first(block(prv)), first(full_b), dev(prv))
            self.down = links.copy(second(block(prv)), second(full_b), dev(prv))
        self.up_plain = links.copy(second(block(nxt)), second(full_a), dev(nxt))
        self.up = links.copy(first(block(nxt)), first(full_a), dev(nxt))

    def begin(self):
        if self.n == 4:
            self.links.start(self.far_up)
            self.links.start(self.far_down)
            self.links.start(self.up_plain)
            self.links.start(self.down_plain)
        elif self.n == 2:
            self.links.start(self.up_plain)
            self.links.start(self.up)

    def relay(self):
        if self.n == 4:
            self.far_up.wait_recv()
            part = self.first(self.block(self.nxt))
            part[...] = (part[...].astype(F32) + self.half_a[...].astype(F32)).astype(BF16)
            self.links.start(self.up)
            self.far_down.wait_recv()
            part = self.second(self.block(self.prv))
            part[...] = (part[...].astype(F32) + self.half_b[...].astype(F32)).astype(BF16)
            self.links.start(self.down)

    def end(self):
        total = self.block(self.c)[...].astype(F32)
        if self.n > 1:
            self.up_plain.wait_recv()
            self.up.wait_recv()
            total = total + self.full_a[...].astype(F32)
        if self.n == 4:
            self.down_plain.wait_recv()
            self.down.wait_recv()
            total = total + self.full_b[...].astype(F32)
        return total


class SumPlane:

    def __init__(self, links, nx, ny, x, y, at_x, at_y, part, bufs):
        rows = part.shape[2]
        h = rows // 2
        q = h // 2
        (ha, hb, fa, fb, sa, ga, gb, ea, eb) = bufs[:9]
        (hc, hd, fc, fd, sb, gc, gd, ec, ed) = bufs[9:]
        self.sa, self.sb = sa, sb

        def wide_first(r):
            return r.at[:, pl.ds(0, q), :]

        def wide_second(r):
            return r.at[:, pl.ds(q, q), :]

        def flat_first(r):
            return r.at[pl.ds(0, q), :]

        def flat_second(r):
            return r.at[pl.ds(q, q), :]

        self.a1 = SumLine(
            links, nx, x, at_x, lambda c: part.at[:, c, pl.ds(0, h), :], wide_first, wide_second, ha, hb, fa, fb
        )
        self.b1 = SumLine(
            links, ny, y, at_y, lambda c: part.at[c, :, pl.ds(h, h), :], wide_first, wide_second, hc, hd, fc, fd
        )
        self.a2 = SumLine(links, ny, y, at_y, lambda c: sa.at[c], flat_first, flat_second, ga, gb, ea, eb)
        self.b2 = SumLine(links, nx, x, at_x, lambda c: sb.at[c], flat_first, flat_second, gc, gd, ec, ed)

    def steps(self, done):
        def begin():
            self.a1.begin()
            self.b1.begin()

        def relay():
            self.a1.relay()
            self.b1.relay()

        def turn():
            self.sa[...] = self.a1.end().astype(BF16)
            self.a2.begin()
            self.sb[...] = self.b1.end().astype(BF16)
            self.b2.begin()

        def relay2():
            self.a2.relay()
            self.b2.relay()

        def end():
            done(self.a2.end(), self.b2.end())

        return [begin, relay, turn, relay2, end]


def sum_buffers(nx, ny, rows):
    h = rows // 2
    q = h // 2

    def v(*shape):
        return pltpu.VMEM((*shape, LANES), BF16)

    return [
        v(ny, q), v(ny, q), v(ny, h), v(ny, h), v(ny, h), v(q), v(q), v(h), v(h),
        v(nx, q), v(nx, q), v(nx, h), v(nx, h), v(nx, h), v(q), v(q), v(h), v(h),
    ]


SEM_LIMIT = 300


def kernel(cfg, *refs):
    (nz, nx, ny, cap, slots, moe_at) = cfg
    (q_h, k_h, v_h, gates_h, mixw_h, rows_h, rids_t, group_t, inner_t, gain, wg_h, wu_h, wd_h) = refs[:13]
    (out_mix, out_moe) = refs[13:15]
    (
        k_all, v_all, q_v, gk, acc, top,
        mixw, mix_part, att,
        rows_v, wg, wu, wd,
        disp, arrived, feats, part, back, ret, table,
        sems, dsem_s, dsem_r, rsem_s, rsem_r, lsem,
    ) = refs[15:41]
    mix_bufs = refs[41:59]
    moe_bufs = refs[59:77]

    ep_n, tp_n = 2 * nz, nx * ny
    ep, tp = lax.axis_index("ep"), lax.axis_index("tp")
    z, core = ep // 2, ep % 2
    y, x = tp // nx, tp % nx
    rows_a = q_h.shape[0]
    rows_m = rows_h.shape[0]
    width = rows_h.shape[1]
    experts = ep_n
    held = experts * cap
    links = Links(sems, SEM_LIMIT)

    def at_ep(p):
        return {"ep": p}

    def at_x(c):
        return {"tp": y * nx + c}

    def at_y(c):
        return {"tp": c * nx + x}

    own_rows = pl.ds(pl.multiple_of(core * rows_a, rows_a), rows_a)

    def mine(buf, chip):
        return buf.at[chip, own_rows, :]

    loads = [
        pltpu.make_async_copy(src, dst, lsem.at[i])
        for i, (src, dst) in enumerate(
            [
                (rows_h, rows_v),
                (k_h, mine(k_all, z)),
                (v_h, mine(v_all, z)),
                (q_h, q_v),
                (gates_h, gk),
                (wg_h, wg),
                (wu_h, wu),
                (wd_h, wd),
                (mixw_h, mixw),
            ]
        )
    ]
    for c in loads:
        c.start()

    if cap % 16:
        whole = cap // 16 * 16
        arrived[:, whole:, :] = jnp.zeros((experts, slots - whole, LANES), BF16)
        ret[:, whole:, :] = jnp.zeros((experts, slots - whole, LANES), BF16)

    barrier = pltpu.get_barrier_semaphore()

    def greet(o, carry):
        pl.semaphore_signal(barrier, inc=1, device_id=at_ep((ep + o) % ep_n), device_id_type=MESH)
        return carry

    lax.fori_loop(1, ep_n, greet, 0)
    for o in range(1, nx):
        pl.semaphore_signal(barrier, inc=1, device_id=at_x((x + o) % nx), device_id_type=MESH)
    for o in range(1, ny):
        pl.semaphore_signal(barrier, inc=1, device_id=at_y((y + o) % ny), device_id_type=MESH)

    table[...] = jnp.zeros(table.shape, F32)
    loads[0].wait()
    ids_t = rids_t[...].astype(F32)
    expert_rows = lax.broadcasted_iota(jnp.int32, (experts, rows_m), 0).astype(F32)
    hit0, hit1 = ids_t[0:1] == expert_rows, ids_t[1:2] == expert_rows
    before = one_hot(
        lax.broadcasted_iota(jnp.int32, (rows_m, rows_m), 0)
        < lax.broadcasted_iota(jnp.int32, (rows_m, rows_m), 1)
    )
    rank = jnp.dot(one_hot(hit0 | hit1), before, preferred_element_type=F32)
    slot0 = ids_t[0:1] * slots + jnp.sum(jnp.where(hit0, rank, 0.0), axis=0, keepdims=True)
    slot1 = ids_t[1:2] * slots + jnp.sum(jnp.where(hit1, rank, 0.0), axis=0, keepdims=True)
    gates_in = inner_t[...]
    share = group_t[...] * gates_in / jnp.sum(gates_in, axis=0, keepdims=True)
    for k, row in enumerate((slot0, slot1, share[0:1], share[1:2])):
        table[k : k + 1, 0:rows_m] = row
    slot_rows = lax.broadcasted_iota(jnp.int32, (experts * slots, rows_m), 0).astype(F32)
    select = one_hot((slot_rows == slot0) | (slot_rows == slot1))
    squares = jnp.zeros((rows_m, LANES), F32)
    for b in range(width // LANES):
        r = rows_v[:, b * LANES : (b + 1) * LANES].astype(F32)
        squares = squares + r * r
    mean = jnp.sum(squares, axis=1, keepdims=True) / width
    own_cols = pl.ds(pl.multiple_of(tp * LANES, LANES), LANES)
    normed = (rows_v[:, own_cols].astype(F32) * lax.rsqrt(mean + NORM_EPS) * gain[:, own_cols]).astype(BF16)
    disp[...] = (
        jnp.dot(select, normed, preferred_element_type=F32).astype(BF16).reshape(experts, slots, LANES)
    )

    loads[1].wait()
    loads[2].wait()
    pl.semaphore_wait(barrier, ep_n - 1 + nx - 1 + ny - 1)

    used = pl.ds(0, cap)

    def dispatch_copy(o):
        peer = (ep + o) % ep_n
        return pltpu.make_async_remote_copy(
            src_ref=disp.at[peer, used, :],
            dst_ref=arrived.at[ep, used, :],
            send_sem=dsem_s.at[o],
            recv_sem=dsem_r.at[o],
            device_id=at_ep(peer),
            device_id_type=MESH,
        )

    def return_copy(o):
        peer = (ep + o) % ep_n
        return pltpu.make_async_remote_copy(
            src_ref=back.at[peer, used, :],
            dst_ref=ret.at[ep, used, :],
            send_sem=rsem_s.at[o],
            recv_sem=rsem_r.at[o],
            device_id=at_ep(peer),
            device_id_type=MESH,
        )

    def each_peer(do):
        def step(o, carry):
            do(o)
            return carry

        lax.fori_loop(1, ep_n, step, 0)

    each_peer(lambda o: dispatch_copy(o).start())

    up_chip = at_ep(((z + 1) % nz) * 2 + core)
    down_chip = at_ep(((z + nz - 1) % nz) * 2 + core)
    partner = at_ep(z * 2 + 1 - core)
    half = nz // 2
    reach = {"k_up": half, "k_down": half - 1, "v_up": half - 1, "v_down": half}
    ring, cross = {}, {}
    for kind in ("k", "v"):
        buf = k_all if kind == "k" else v_all
        cross[kind, 0] = links.copy(mine(buf, z), mine(buf, z), partner)
        for way, sign, dev in (("up", -1, up_chip), ("down", 1, down_chip)):
            for d in range(1, reach[kind + "_" + way] + 1):
                sent = (z + sign * (d - 1) + nz) % nz
                got = (z + sign * d + nz) % nz
                ring[kind, way, d] = links.copy(mine(buf, sent), mine(buf, sent), dev)
                cross[kind, way, d] = links.copy(mine(buf, got), mine(buf, got), partner)

    for kind in ("k", "v"):
        for way in ("up", "down"):
            if (kind, way, 1) in ring:
                links.start(ring[kind, way, 1])
        links.start(cross[kind, 0])

    arrived[ep] = disp[ep]

    def gates_of(chip, start, size):
        return gk[:, pl.ds(pl.multiple_of(chip * 2 * rows_a + start, rows_a), size)]

    scale = LOG2E * LANES**-0.5
    chunk = 2 * rows_a
    q_block = min(256, rows_a)
    top[...] = jnp.full(top.shape, LOW_SCORE, F32)
    acc[...] = jnp.zeros(acc.shape, F32)
    loads[3].wait()
    loads[4].wait()
    base = jnp.max(gates_of(z, core * rows_a, rows_a), axis=1, keepdims=True)

    def attend(chip, masked):
        bias = (gates_of(chip, 0, chunk) - base) * LOG2E
        ones = jnp.ones((chunk, LANES), BF16)
        for i in range(rows_a // q_block):
            here = pl.ds(i * q_block, q_block)
            scores = (
                lax.dot_general(
                    q_v[here, :], k_all[chip], (((1,), (1,)), ((), ())), preferred_element_type=F32
                )
                * scale
                - bias
            )
            if masked:
                key_pos = lax.broadcasted_iota(jnp.int32, (q_block, chunk), 1)
                query_pos = lax.broadcasted_iota(jnp.int32, (q_block, chunk), 0) + core * rows_a + i * q_block
                scores = jnp.where(key_pos <= query_pos, scores, LOW_SCORE)
            old = top[here, :]
            new = jnp.maximum(old, jnp.max(scores, axis=1, keepdims=True))
            top[here, :] = new
            shrink = jnp.exp2(old - new)
            weights = jnp.exp2(scores - new[:, 0:1]).astype(BF16)
            both = jnp.concatenate([v_all[chip], ones], axis=1)
            add = jnp.dot(weights, both, preferred_element_type=F32)
            acc[here, :] = acc[here, :] * jnp.concatenate([shrink, shrink], axis=1) + add

    gather = {}
    h, qtr = held // 2, held // 4
    gather["a1"] = GatherLine(
        links, nx, x, at_x, lambda c: feats.at[y, c, pl.ds(0, h), :],
        lambda r: r.at[pl.ds(0, qtr), :], lambda r: r.at[pl.ds(qtr, qtr), :],
    )
    gather["b1"] = GatherLine(
        links, ny, y, at_y, lambda c: feats.at[c, x, pl.ds(h, h), :],
        lambda r: r.at[pl.ds(0, qtr), :], lambda r: r.at[pl.ds(qtr, qtr), :],
    )
    gather["a2"] = GatherLine(
        links, ny, y, at_y, lambda c: feats.at[c, :, pl.ds(0, h), :],
        lambda r: r.at[:, pl.ds(0, qtr), :], lambda r: r.at[:, pl.ds(qtr, qtr), :],
    )
    gather["b2"] = GatherLine(
        links, nx, x, at_x, lambda c: feats.at[:, c, pl.ds(h, h), :],
        lambda r: r.at[:, pl.ds(0, qtr), :], lambda r: r.at[:, pl.ds(qtr, qtr), :],
    )

    def packed_row(shape, dim):
        i = lax.broadcasted_iota(jnp.int32, shape, dim)
        return (i // cap) * slots + i % cap

    def moe_arrive():
        each_peer(lambda o: dispatch_copy(o).wait_recv())
        where_from = packed_row((held, 1), 0)
        pick = one_hot(where_from == lax.broadcasted_iota(jnp.int32, (held, experts * slots), 1))
        feats[y, x] = jnp.dot(
            pick, arrived[...].reshape(experts * slots, LANES), preferred_element_type=F32
        ).astype(BF16)
        gather["a1"].begin()
        gather["b1"].begin()

    def moe_gather_relay():
        gather["a1"].relay()
        gather["b1"].relay()

    def moe_gather_turn():
        gather["a1"].end()
        gather["a2"].begin()
        gather["b1"].end()
        gather["b2"].begin()

    def moe_gather_relay2():
        gather["a2"].relay()
        gather["b2"].relay()

    made = {"gate": 0.0, "up": 0.0}

    def moe_gathered():
        gather["a2"].end()
        gather["b2"].end()
        loads[5].wait()
        loads[6].wait()

    def moe_hidden(part_rows):
        for yy in part_rows:
            block = jnp.concatenate([feats[yy, xx] for xx in range(nx)], axis=1)
            cols = slice(yy * nx * LANES, (yy + 1) * nx * LANES)
            made["gate"] = made["gate"] + jnp.dot(block, wg[cols, :], preferred_element_type=F32)
            made["up"] = made["up"] + jnp.dot(block, wu[cols, :], preferred_element_type=F32)

    def moe_act():
        gate = made["gate"]
        made["hidden"] = (gate / (1.0 + jnp.exp(-gate)) * made["up"]).astype(BF16)

    def project(rows, weights_ref, dest, start=0, stop=tp_n):
        for b in range(start, stop, 2):
            both = jnp.dot(rows, weights_ref[:, b * LANES : (b + 2) * LANES], preferred_element_type=F32)
            for e in (0, 1):
                dest[(b + e) // nx, (b + e) % nx] = both[:, e * LANES : (e + 1) * LANES].astype(BF16)

    def expert_done(first, second):
        packed = jnp.concatenate([first, second], axis=0).astype(BF16)
        where_to = packed_row((1, held), 1)
        spread = one_hot(lax.broadcasted_iota(jnp.int32, (experts * slots, held), 0) == where_to)
        back[...] = (
            jnp.dot(spread, packed, preferred_element_type=F32).astype(BF16).reshape(experts, slots, LANES)
        )
        each_peer(lambda o: return_copy(o).start())
        ret[ep] = back[ep]

    expert_sum = SumPlane(links, nx, ny, x, y, at_x, at_y, part, moe_bufs).steps(expert_done)

    def moe_down(start, stop):
        project(made["hidden"], wd, part, start, stop)

    def moe_combine():
        each_peer(lambda o: return_copy(o).wait_recv())
        columns = table[...].T[0:rows_m]
        slot_cols = lax.broadcasted_iota(jnp.int32, (rows_m, experts * slots), 1).astype(F32)
        rows = ret[...].reshape(experts * slots, LANES)
        total = 0.0
        for k in (0, 1):
            hit = one_hot(slot_cols == columns[:, k : k + 1])
            total = total + columns[:, k + 2 : k + 3] * jnp.dot(hit, rows, preferred_element_type=F32)
        out_moe[...] = total.astype(BF16)

    mid_y, mid_t = (ny + 1) // 2, (tp_n // 2 + 1) // 2 * 2
    moe = [
        moe_arrive,
        moe_gather_relay,
        moe_gather_turn,
        moe_gather_relay2,
        lambda: (moe_gathered(), moe_hidden(range(mid_y))),
        lambda: (moe_hidden(range(mid_y, ny)), moe_act()),
        lambda: (loads[7].wait(), moe_down(0, mid_t)),
        lambda: (moe_down(mid_t, tp_n), expert_sum[0]()),
        expert_sum[1],
        expert_sum[2],
        expert_sum[3],
        expert_sum[4],
        moe_combine,
    ]
    moe_at = list(moe_at)
    assert len(moe_at) == len(moe)

    def moe_slot(number):
        while moe_at and moe_at[0] <= number:
            moe_at.pop(0)
            moe.pop(0)()

    cross["k", 0].wait_recv()
    cross["v", 0].wait_recv()
    attend(z, True)

    def pass_on(kind, d):
        for way in ("up", "down"):
            if (kind, way, d) in ring:
                ring[kind, way, d].wait_recv()
                if (kind, way, d + 1) in ring:
                    links.start(ring[kind, way, d + 1])
                links.start(cross[kind, way, d])

    def landed(d):
        for kind in ("k", "v"):
            for way in ("up", "down"):
                if (kind, way, d) in ring:
                    cross[kind, way, d].wait_recv()

    def attend_up(d):
        @pl.when(z >= d)
        def _():
            attend(z - d, False)

    def attend_down(d):
        @pl.when(z + d >= nz)
        def _():
            attend(z + d - nz, False)

    for d in range(1, half + 1):
        pass_on("k", d)
        if d > 1:
            landed(d - 1)
            attend_up(d - 1)
        moe_slot(2 * d - 1)
        pass_on("v", d)
        if d > 1:
            attend_down(d - 1)
        moe_slot(2 * d)
    landed(half)
    attend_up(half)

    att[...] = (acc[:, 0:LANES] / acc[:, LANES:]).astype(BF16)

    def mix_done(first, second):
        out_mix[pl.ds(0, rows_a // 2), :] = first.astype(BF16)
        out_mix[pl.ds(rows_a // 2, rows_a // 2), :] = second.astype(BF16)

    mix = SumPlane(links, nx, ny, x, y, at_x, at_y, mix_part, mix_bufs).steps(mix_done)
    loads[8].wait()
    project(att[...], mixw, mix_part)
    for k, step in enumerate(mix):
        step()
        moe_slot(100 + k)
    moe_slot(1000)
    links.finish()
    each_peer(lambda o: dispatch_copy(o).wait_send())
    each_peer(lambda o: return_copy(o).wait_send())


def body(sizes, moe_at, queries, keys, values, log_gate_sums, mixer_weight, moe_rows, route_ids,
         group_gate, inner_gate, norm_gain, gate_weight, up_weight, down_weight):
    nz, nx, ny = sizes
    rows_a, rows_m, width = queries.shape[0], moe_rows.shape[0], moe_rows.shape[1]
    experts = 2 * nz
    cap = 3 * rows_m * route_ids.shape[1] // (2 * experts)
    slots = -(-cap // 16) * 16
    hidden = gate_weight.shape[2]
    held = experts * cap

    def v(*shape, dtype=BF16):
        return pltpu.VMEM(shape, dtype)

    scratch = [
        v(nz, 2 * rows_a, LANES), v(nz, 2 * rows_a, LANES), v(rows_a, LANES), v(1, nz * 2 * rows_a, dtype=F32),
        v(rows_a, 2 * LANES, dtype=F32), v(rows_a, LANES, dtype=F32),
        v(LANES, width), v(ny, nx, rows_a, LANES), v(rows_a, LANES),
        v(rows_m, width), v(width, hidden), v(width, hidden), v(hidden, width),
        v(experts, slots, LANES), v(experts, slots, LANES), v(ny, nx, held, LANES), v(ny, nx, held, LANES),
        v(experts, slots, LANES), v(experts, slots, LANES), v(LANES, -(-rows_m // LANES) * LANES, dtype=F32),
        pltpu.SemaphoreType.DMA((SEM_LIMIT,)),
        pltpu.SemaphoreType.DMA((2 * nz,)), pltpu.SemaphoreType.DMA((2 * nz,)),
        pltpu.SemaphoreType.DMA((2 * nz,)), pltpu.SemaphoreType.DMA((2 * nz,)),
        pltpu.SemaphoreType.DMA((9,)),
        *sum_buffers(nx, ny, rows_a),
        *sum_buffers(nx, ny, held),
    ]
    hbm = pl.BlockSpec(memory_space=pl.ANY)
    vm = pl.BlockSpec(memory_space=pltpu.VMEM)
    return pl.pallas_call(
        functools.partial(kernel, (nz, nx, ny, cap, slots, moe_at)),
        out_shape=(
            jax.ShapeDtypeStruct((rows_a, LANES), BF16),
            jax.ShapeDtypeStruct((rows_m, LANES), BF16),
        ),
        in_specs=[hbm] * 6 + [vm] * 4 + [hbm] * 3,
        out_specs=(vm, vm),
        scratch_shapes=scratch,
        compiler_params=pltpu.CompilerParams(
            collective_id=0, has_side_effects=True, vmem_limit_bytes=60 * 1024 * 1024
        ),
        name="step",
    )(
        queries, keys, values, log_gate_sums.T, mixer_weight, moe_rows, route_ids.T,
        group_gate.reshape(1, -1), inner_gate.T, norm_gain.reshape(1, -1), gate_weight[0], up_weight[0], down_weight[0],
    )


MOE_AT = (3, 4, 5, 7, 9, 9, 10, 11, 13, 15, 16, 100, 103)


def plane_of(tp):
    side = 1
    while side * side < tp:
        side *= 2
    return side, tp // side


def solution(mesh, plane=None, moe_at=MOE_AT):
    nx, ny = plane or plane_of(mesh.shape["tp"])
    sizes = (mesh.shape["ep"] // 2, nx, ny)
    return jax.shard_map(
        functools.partial(body, sizes, moe_at),
        mesh=mesh,
        in_specs=(
            P("ep", "tp"),
            P("ep", "tp"),
            P("ep", "tp"),
            P(None, "tp"),
            P("tp", None),
            P("ep", None),
            P("ep", None),
            P("ep"),
            P("ep", None),
            P(),
            P("ep", None, "tp"),
            P("ep", None, "tp"),
            P("ep", "tp", None),
        ),
        out_specs=(P("ep", "tp"), P("ep", "tp")),
        check_vma=False,
    )
```

```python
import functools

import jax
import jax.numpy as jnp
from jax import lax
from jax.experimental import pallas as pl
from jax.experimental.pallas import tpu as pltpu
from jax.sharding import PartitionSpec as P

LOW_SCORE = -1e30
NORM_EPS = 1e-06
LOG2E = 1.4426950408889634
LANES = 128
MESH = pl.DeviceIdType.MESH
F32 = jnp.float32
BF16 = jnp.bfloat16


def one_hot(mask):
    return jnp.where(mask, 1.0, 0.0).astype(BF16)


class Links:

    def __init__(self, sems, limit):
        self.sems, self.limit, self.used, self.sent = sems, limit, 0, []

    def new(self):
        self.used += 1
        assert self.used <= self.limit
        return self.sems.at[self.used - 1]

    def copy(self, src, dst, device):
        c = pltpu.make_async_remote_copy(
            src_ref=src,
            dst_ref=dst,
            send_sem=self.new(),
            recv_sem=self.new(),
            device_id=device,
            device_id_type=MESH,
        )
        return c

    def start(self, c):
        c.start()
        self.sent.append(c)

    def finish(self):
        for c in self.sent:
            c.wait_send()
        self.sent = []


class GatherLine:

    def __init__(self, links, n, c, dev, block, first, second):
        self.links, self.n = links, n
        nxt, prv = (c + 1) % n, (c + n - 1) % n
        if n == 1:
            return

        def same(ref, to):
            return links.copy(ref, ref, dev(to))

        self.up = [same(first(block(c)), nxt), same(second(block(c)), nxt)]
        self.down = []
        if n == 4:
            self.down = [same(second(block(c)), prv), same(first(block(c)), prv)]
            self.relay_up = same(first(block(prv)), nxt)
            self.relay_down = same(second(block(nxt)), prv)

    def begin(self):
        if self.n == 1:
            return
        for k in (0, 1):
            self.links.start(self.up[k])
            if self.n == 4:
                self.links.start(self.down[k])

    def relay(self):
        if self.n == 4:
            self.up[0].wait_recv()
            self.links.start(self.relay_up)
            self.down[0].wait_recv()
            self.links.start(self.relay_down)

    def near(self):
        if self.n == 2:
            self.up[0].wait_recv()
            self.up[1].wait_recv()
        if self.n == 4:
            self.up[1].wait_recv()
            self.down[1].wait_recv()

    def end(self):
        if self.n == 4:
            self.relay_up.wait_recv()
            self.relay_down.wait_recv()


class SumLine:

    def __init__(self, links, n, c, dev, block, first, second, half_a, half_b, full_a, full_b):
        self.links, self.n, self.c, self.block = links, n, c, block
        self.first, self.second = first, second
        self.half_a, self.half_b, self.full_a, self.full_b = half_a, half_b, full_a, full_b
        nxt, prv, far = (c + 1) % n, (c + n - 1) % n, (c + 2) % n
        self.nxt, self.prv = nxt, prv
        if n == 1:
            return
        if n == 4:
            self.far_up = links.copy(first(block(far)), half_a, dev(nxt))
            self.far_down = links.copy(second(block(far)), half_b, dev(prv))
            self.down_plain = links.copy(first(block(prv)), first(full_b), dev(prv))
            self.down = links.copy(second(block(prv)), second(full_b), dev(prv))
        self.up_plain = links.copy(second(block(nxt)), second(full_a), dev(nxt))
        self.up = links.copy(first(block(nxt)), first(full_a), dev(nxt))

    def begin(self):
        if self.n == 4:
            self.links.start(self.far_up)
            self.links.start(self.far_down)
            self.links.start(self.up_plain)
            self.links.start(self.down_plain)
        elif self.n == 2:
            self.links.start(self.up_plain)
            self.links.start(self.up)

    def begin_part(self, offset):
        if self.n == 4 and offset == 2:
            self.links.start(self.far_up)
            self.links.start(self.far_down)
        if self.n == 4 and offset == 1:
            self.links.start(self.up_plain)
        if self.n == 4 and offset == 3:
            self.links.start(self.down_plain)
        if self.n == 2 and offset == 1:
            self.links.start(self.up_plain)
            self.links.start(self.up)

    def relay(self):
        if self.n == 4:
            self.far_up.wait_recv()
            part = self.first(self.block(self.nxt))
            part[...] = (part[...].astype(F32) + self.half_a[...].astype(F32)).astype(BF16)
            self.links.start(self.up)
            self.far_down.wait_recv()
            part = self.second(self.block(self.prv))
            part[...] = (part[...].astype(F32) + self.half_b[...].astype(F32)).astype(BF16)
            self.links.start(self.down)

    def end(self):
        total = self.block(self.c)[...].astype(F32)
        if self.n > 1:
            self.up_plain.wait_recv()
            self.up.wait_recv()
            total = total + self.full_a[...].astype(F32)
        if self.n == 4:
            self.down_plain.wait_recv()
            self.down.wait_recv()
            total = total + self.full_b[...].astype(F32)
        return total


def spread_order(n):
    return {4: (2, 1, 3, 0), 2: (1, 0), 1: (0,)}[n]


class SumPlane:

    def __init__(self, links, nx, ny, x, y, at_x, at_y, part, bufs):
        rows = part.shape[2]
        h = rows // 2
        q = h // 2

        def first(r):
            return r.at[pl.ds(0, q), :]

        def second(r):
            return r.at[pl.ds(q, q), :]

        def way(n1, c1, at1, n2, c2, at2, block, buf):
            (ha, hb, fa, fb, mid, ga, gb, ea, eb) = buf
            lines = []
            for k, o in enumerate(spread_order(n2)):
                other = (c2 + o) % n2
                line = SumLine(
                    links, n1, c1, at1, functools.partial(block, other), first, second,
                    ha.at[k], hb.at[k], fa.at[k], fb.at[k],
                )
                lines.append((o, other, line))
            last = SumLine(links, n2, c2, at2, lambda c: mid.at[c], first, second, ga, gb, ea, eb)
            return lines, mid, last

        self.ways = [
            way(nx, x, at_x, ny, y, at_y, lambda other, c: part.at[other, c, pl.ds(0, h), :], bufs[:9]),
            way(ny, y, at_y, nx, x, at_x, lambda other, c: part.at[c, other, pl.ds(h, h), :], bufs[9:]),
        ]

    def steps(self, done):
        def begin():
            for k in range(max(len(w[0]) for w in self.ways)):
                for lines, _, _ in self.ways:
                    if k < len(lines):
                        lines[k][2].begin()

        def relay():
            for k in range(max(len(w[0]) for w in self.ways)):
                for lines, _, _ in self.ways:
                    if k < len(lines):
                        lines[k][2].relay()

        def turn():
            for k in range(max(len(w[0]) for w in self.ways)):
                for lines, mid, last in self.ways:
                    if k < len(lines):
                        o, other, line = lines[k]
                        mid[other] = line.end().astype(BF16)
                        last.begin_part(o)

        def relay2():
            for _, _, last in self.ways:
                last.relay()

        def end():
            done(*[last.end() for _, _, last in self.ways])

        return [begin, relay, turn, relay2, end]


def sum_buffers(nx, ny, rows):
    h = rows // 2
    q = h // 2

    def v(*shape):
        return pltpu.VMEM((*shape, LANES), BF16)

    return [
        v(ny, q), v(ny, q), v(ny, h), v(ny, h), v(ny, h), v(q), v(q), v(h), v(h),
        v(nx, q), v(nx, q), v(nx, h), v(nx, h), v(nx, h), v(q), v(q), v(h), v(h),
    ]


SEM_LIMIT = 500


def kernel(cfg, *refs):
    (nz, nx, ny, cap, slots, moe_at) = cfg
    (q_h, k_h, v_h, gates_h, mixw_h, rows_h, rids_t, group_t, inner_t, gain, wg_h, wu_h, wd_h) = refs[:13]
    (out_mix, out_moe) = refs[13:15]
    (
        k_all, v_all, q_v, gk, acc, top,
        mixw, mix_part, att,
        rows_v, wg, wu, wd,
        disp, arrived, feats, part, back, ret, table,
        sems, dsem_s, dsem_r, rsem_s, rsem_r, lsem,
    ) = refs[15:41]
    mix_bufs = refs[41:59]
    moe_bufs = refs[59:77]

    ep_n, tp_n = 2 * nz, nx * ny
    ep, tp = lax.axis_index("ep"), lax.axis_index("tp")
    z, core = ep // 2, ep % 2
    y, x = tp // nx, tp % nx
    rows_a = q_h.shape[0]
    rows_m = rows_h.shape[0]
    width = rows_h.shape[1]
    experts = ep_n
    held = experts * cap
    links = Links(sems, SEM_LIMIT)

    def at_ep(p):
        return {"ep": p}

    def at_x(c):
        return {"tp": y * nx + c}

    def at_y(c):
        return {"tp": c * nx + x}

    own_rows = pl.ds(pl.multiple_of(core * rows_a, rows_a), rows_a)

    def mine(buf, chip):
        return buf.at[chip, own_rows, :]

    loads = [
        pltpu.make_async_copy(src, dst, lsem.at[i])
        for i, (src, dst) in enumerate(
            [
                (rows_h, rows_v),
                (k_h, mine(k_all, z)),
                (v_h, mine(v_all, z)),
                (q_h, q_v),
                (gates_h, gk),
                (wg_h, wg),
                (wu_h, wu),
                (wd_h, wd),
                (mixw_h, mixw),
            ]
        )
    ]
    for c in loads:
        c.start()

    if cap % 16:
        whole = cap // 16 * 16
        arrived[:, whole:, :] = jnp.zeros((experts, slots - whole, LANES), BF16)
        ret[:, whole:, :] = jnp.zeros((experts, slots - whole, LANES), BF16)

    barrier = pltpu.get_barrier_semaphore()

    def greet(o, carry):
        pl.semaphore_signal(barrier, inc=1, device_id=at_ep((ep + o) % ep_n), device_id_type=MESH)
        return carry

    lax.fori_loop(1, ep_n, greet, 0)
    for o in range(1, nx):
        pl.semaphore_signal(barrier, inc=1, device_id=at_x((x + o) % nx), device_id_type=MESH)
    for o in range(1, ny):
        pl.semaphore_signal(barrier, inc=1, device_id=at_y((y + o) % ny), device_id_type=MESH)

    table[...] = jnp.zeros(table.shape, F32)
    loads[0].wait()
    ids_t = rids_t[...].astype(F32)
    expert_rows = lax.broadcasted_iota(jnp.int32, (experts, rows_m), 0).astype(F32)
    hit0, hit1 = ids_t[0:1] == expert_rows, ids_t[1:2] == expert_rows
    before = one_hot(
        lax.broadcasted_iota(jnp.int32, (rows_m, rows_m), 0)
        < lax.broadcasted_iota(jnp.int32, (rows_m, rows_m), 1)
    )
    rank = jnp.dot(one_hot(hit0 | hit1), before, preferred_element_type=F32)
    slot0 = ids_t[0:1] * slots + jnp.sum(jnp.where(hit0, rank, 0.0), axis=0, keepdims=True)
    slot1 = ids_t[1:2] * slots + jnp.sum(jnp.where(hit1, rank, 0.0), axis=0, keepdims=True)
    gates_in = inner_t[...]
    share = group_t[...] * gates_in / jnp.sum(gates_in, axis=0, keepdims=True)
    for k, row in enumerate((slot0, slot1, share[0:1], share[1:2])):
        table[k : k + 1, 0:rows_m] = row
    slot_rows = lax.broadcasted_iota(jnp.int32, (experts * slots, rows_m), 0).astype(F32)
    select = one_hot((slot_rows == slot0) | (slot_rows == slot1))
    squares = jnp.zeros((rows_m, LANES), F32)
    for b in range(width // LANES):
        r = rows_v[:, b * LANES : (b + 1) * LANES].astype(F32)
        squares = squares + r * r
    mean = jnp.sum(squares, axis=1, keepdims=True) / width
    own_cols = pl.ds(pl.multiple_of(tp * LANES, LANES), LANES)
    normed = (rows_v[:, own_cols].astype(F32) * lax.rsqrt(mean + NORM_EPS) * gain[:, own_cols]).astype(BF16)
    disp[...] = (
        jnp.dot(select, normed, preferred_element_type=F32).astype(BF16).reshape(experts, slots, LANES)
    )

    loads[1].wait()
    loads[2].wait()
    pl.semaphore_wait(barrier, ep_n - 1 + nx - 1 + ny - 1)

    used = pl.ds(0, cap)

    def dispatch_copy(o):
        peer = (ep + o) % ep_n
        return pltpu.make_async_remote_copy(
            src_ref=disp.at[peer, used, :],
            dst_ref=arrived.at[ep, used, :],
            send_sem=dsem_s.at[o],
            recv_sem=dsem_r.at[o],
            device_id=at_ep(peer),
            device_id_type=MESH,
        )

    def return_copy(o):
        peer = (ep + o) % ep_n
        return pltpu.make_async_remote_copy(
            src_ref=back.at[peer, used, :],
            dst_ref=ret.at[ep, used, :],
            send_sem=rsem_s.at[o],
            recv_sem=rsem_r.at[o],
            device_id=at_ep(peer),
            device_id_type=MESH,
        )

    def each_peer(do):
        def step(o, carry):
            do(o)
            return carry

        lax.fori_loop(1, ep_n, step, 0)

    each_peer(lambda o: dispatch_copy(o).start())

    up_chip = at_ep(((z + 1) % nz) * 2 + core)
    down_chip = at_ep(((z + nz - 1) % nz) * 2 + core)
    partner = at_ep(z * 2 + 1 - core)
    half = nz // 2
    reach = {"k_up": half, "k_down": half - 1, "v_up": half - 1, "v_down": half}
    ring, cross = {}, {}
    for kind in ("k", "v"):
        buf = k_all if kind == "k" else v_all
        cross[kind, 0] = links.copy(mine(buf, z), mine(buf, z), partner)
        for way, sign, dev in (("up", -1, up_chip), ("down", 1, down_chip)):
            for d in range(1, reach[kind + "_" + way] + 1):
                sent = (z + sign * (d - 1) + nz) % nz
                got = (z + sign * d + nz) % nz
                ring[kind, way, d] = links.copy(mine(buf, sent), mine(buf, sent), dev)
                cross[kind, way, d] = links.copy(mine(buf, got), mine(buf, got), partner)

    for kind in ("k", "v"):
        for way in ("up", "down"):
            if (kind, way, 1) in ring:
                links.start(ring[kind, way, 1])
        links.start(cross[kind, 0])

    arrived[ep] = disp[ep]

    def gates_of(chip, start, size):
        return gk[:, pl.ds(pl.multiple_of(chip * 2 * rows_a + start, rows_a), size)]

    scale = LOG2E * LANES**-0.5
    chunk = 2 * rows_a
    q_block = min(256, rows_a)
    top[...] = jnp.full(top.shape, LOW_SCORE, F32)
    acc[...] = jnp.zeros(acc.shape, F32)
    loads[3].wait()
    loads[4].wait()
    base = jnp.max(gates_of(z, core * rows_a, rows_a), axis=1, keepdims=True)

    def attend(chip, masked):
        bias = (gates_of(chip, 0, chunk) - base) * LOG2E
        ones = jnp.ones((chunk, LANES), BF16)
        def query_rows(i):
            here = pl.ds(i * q_block, q_block)
            scores = (
                lax.dot_general(
                    q_v[here, :], k_all[chip], (((1,), (1,)), ((), ())), preferred_element_type=F32
                )
                * scale
                - bias
            )
            if masked:
                key_pos = lax.broadcasted_iota(jnp.int32, (q_block, chunk), 1)
                query_pos = lax.broadcasted_iota(jnp.int32, (q_block, chunk), 0) + core * rows_a + i * q_block
                scores = jnp.where(key_pos <= query_pos, scores, LOW_SCORE)
            old = top[here, :]
            new = jnp.maximum(old, jnp.max(scores, axis=1, keepdims=True))
            top[here, :] = new
            shrink = jnp.exp2(old - new)
            weights = jnp.exp2(scores - new[:, 0:1]).astype(BF16)
            both = jnp.concatenate([v_all[chip], ones], axis=1)
            add = jnp.dot(weights, both, preferred_element_type=F32)
            acc[here, :] = acc[here, :] * jnp.concatenate([shrink, shrink], axis=1) + add

        for i in range(rows_a // q_block):
            query_rows(i)

    gather = {}
    h, qtr = held // 2, held // 4
    gather["a1"] = GatherLine(
        links, nx, x, at_x, lambda c: feats.at[y, c, pl.ds(0, h), :],
        lambda r: r.at[pl.ds(0, qtr), :], lambda r: r.at[pl.ds(qtr, qtr), :],
    )
    gather["b1"] = GatherLine(
        links, ny, y, at_y, lambda c: feats.at[c, x, pl.ds(h, h), :],
        lambda r: r.at[pl.ds(0, qtr), :], lambda r: r.at[pl.ds(qtr, qtr), :],
    )

    def upper(r):
        return r.at[pl.ds(0, qtr), :]

    def lower(r):
        return r.at[pl.ds(qtr, qtr), :]

    def second_line(n1, c1, n2, c2, dev, block):
        lines = {}
        for o in range(n1):
            lines[o] = GatherLine(links, n2, c2, dev, functools.partial(block, (c1 + o) % n1), upper, lower)
        return lines

    gather["a2"] = second_line(nx, x, ny, y, at_y, lambda other, c: feats.at[c, other, pl.ds(0, h), :])
    gather["b2"] = second_line(ny, y, nx, x, at_x, lambda other, c: feats.at[other, c, pl.ds(h, h), :])

    def second_stage(offsets, do):
        for o in offsets:
            for key in ("a2", "b2"):
                if o in gather[key]:
                    do(gather[key][o])

    def packed_row(shape, dim):
        i = lax.broadcasted_iota(jnp.int32, shape, dim)
        return (i // cap) * slots + i % cap

    def moe_arrive():
        each_peer(lambda o: dispatch_copy(o).wait_recv())
        where_from = packed_row((held, 1), 0)
        pick = one_hot(where_from == lax.broadcasted_iota(jnp.int32, (held, experts * slots), 1))
        feats[y, x] = jnp.dot(
            pick, arrived[...].reshape(experts * slots, LANES), preferred_element_type=F32
        ).astype(BF16)
        gather["a1"].begin()
        gather["b1"].begin()
        second_stage((0,), GatherLine.begin)

    def near_offsets(n):
        return {4: (1, 3), 2: (1,), 1: ()}[n]

    def moe_gather_relay():
        gather["a1"].relay()
        gather["b1"].relay()
        for key, n in (("a", nx), ("b", ny)):
            gather[key + "1"].near()
            for o in near_offsets(n):
                gather[key + "2"][o].begin()

    def moe_gather_turn():
        for key, n in (("a", nx), ("b", ny)):
            gather[key + "1"].end()
            if n == 4:
                gather[key + "2"][2].begin()
        second_stage((0,), GatherLine.relay)

    def moe_gather_relay2():
        second_stage((1, 3, 2), GatherLine.relay)

    made = {"gate": 0.0, "up": 0.0}

    def moe_gathered():
        second_stage((0, 1, 3, 2), lambda line: (line.near(), line.end()))
        loads[5].wait()
        loads[6].wait()

    def moe_hidden(part_rows):
        for yy in part_rows:
            block = jnp.concatenate([feats[yy, xx] for xx in range(nx)], axis=1)
            cols = slice(yy * nx * LANES, (yy + 1) * nx * LANES)
            made["gate"] = made["gate"] + jnp.dot(block, wg[cols, :], preferred_element_type=F32)
            made["up"] = made["up"] + jnp.dot(block, wu[cols, :], preferred_element_type=F32)

    def moe_act():
        gate = made["gate"]
        made["hidden"] = (gate / (1.0 + jnp.exp(-gate)) * made["up"]).astype(BF16)

    def project(rows, weights_ref, dest, start=0, stop=tp_n):
        for b in range(start, stop, 2):
            both = jnp.dot(rows, weights_ref[:, b * LANES : (b + 2) * LANES], preferred_element_type=F32)
            for e in (0, 1):
                dest[(b + e) // nx, (b + e) % nx] = both[:, e * LANES : (e + 1) * LANES].astype(BF16)

    def expert_done(first, second):
        packed = jnp.concatenate([first, second], axis=0).astype(BF16)
        where_to = packed_row((1, held), 1)
        spread = one_hot(lax.broadcasted_iota(jnp.int32, (experts * slots, held), 0) == where_to)
        back[...] = (
            jnp.dot(spread, packed, preferred_element_type=F32).astype(BF16).reshape(experts, slots, LANES)
        )
        each_peer(lambda o: return_copy(o).start())
        ret[ep] = back[ep]

    expert_sum = SumPlane(links, nx, ny, x, y, at_x, at_y, part, moe_bufs).steps(expert_done)

    def moe_down(start, stop):
        project(made["hidden"], wd, part, start, stop)

    def moe_combine():
        each_peer(lambda o: return_copy(o).wait_recv())
        columns = table[...].T[0:rows_m]
        slot_cols = lax.broadcasted_iota(jnp.int32, (rows_m, experts * slots), 1).astype(F32)
        rows = ret[...].reshape(experts * slots, LANES)
        total = 0.0
        for k in (0, 1):
            hit = one_hot(slot_cols == columns[:, k : k + 1])
            total = total + columns[:, k + 2 : k + 3] * jnp.dot(hit, rows, preferred_element_type=F32)
        out_moe[...] = total.astype(BF16)

    mid_y, mid_t = (ny + 1) // 2, (tp_n // 2 + 1) // 2 * 2
    moe = [
        moe_arrive,
        moe_gather_relay,
        moe_gather_turn,
        moe_gather_relay2,
        lambda: (moe_gathered(), moe_hidden(range(mid_y))),
        lambda: (moe_hidden(range(mid_y, ny)), moe_act()),
        lambda: (loads[7].wait(), moe_down(0, mid_t)),
        lambda: (moe_down(mid_t, tp_n), expert_sum[0]()),
        expert_sum[1],
        expert_sum[2],
        expert_sum[3],
        expert_sum[4],
        moe_combine,
    ]
    moe_at = list(moe_at)
    assert len(moe_at) == len(moe)

    def moe_slot(number):
        while moe_at and moe_at[0] <= number:
            moe_at.pop(0)
            moe.pop(0)()

    cross["k", 0].wait_recv()
    cross["v", 0].wait_recv()
    attend(z, True)

    def pass_on(kind, d):
        for way in ("up", "down"):
            if (kind, way, d) in ring:
                ring[kind, way, d].wait_recv()
                if (kind, way, d + 1) in ring:
                    links.start(ring[kind, way, d + 1])
                links.start(cross[kind, way, d])

    def landed(d):
        for kind in ("k", "v"):
            for way in ("up", "down"):
                if (kind, way, d) in ring:
                    cross[kind, way, d].wait_recv()

    def attend_up(d):
        @pl.when(z >= d)
        def _():
            attend(z - d, False)

    def attend_down(d):
        @pl.when(z + d >= nz)
        def _():
            attend(z + d - nz, False)

    for d in range(1, half + 1):
        pass_on("k", d)
        moe_slot(4 * d - 3)
        if d > 1:
            landed(d - 1)
            attend_up(d - 1)
        moe_slot(4 * d - 2)
        pass_on("v", d)
        moe_slot(4 * d - 1)
        if d > 1:
            attend_down(d - 1)
        moe_slot(4 * d)
    landed(half)
    attend_up(half)

    att[...] = (acc[:, 0:LANES] / acc[:, LANES:]).astype(BF16)

    def mix_done(first, second):
        out_mix[pl.ds(0, rows_a // 2), :] = first.astype(BF16)
        out_mix[pl.ds(rows_a // 2, rows_a // 2), :] = second.astype(BF16)

    mix = SumPlane(links, nx, ny, x, y, at_x, at_y, mix_part, mix_bufs).steps(mix_done)
    loads[8].wait()
    project(att[...], mixw, mix_part)
    for k, step in enumerate(mix):
        step()
        moe_slot(100 + k)
    moe_slot(1000)
    links.finish()
    each_peer(lambda o: dispatch_copy(o).wait_send())
    each_peer(lambda o: return_copy(o).wait_send())


def body(sizes, moe_at, queries, keys, values, log_gate_sums, mixer_weight, moe_rows, route_ids,
         group_gate, inner_gate, norm_gain, gate_weight, up_weight, down_weight):
    nz, nx, ny = sizes
    rows_a, rows_m, width = queries.shape[0], moe_rows.shape[0], moe_rows.shape[1]
    experts = 2 * nz
    cap = 3 * rows_m * route_ids.shape[1] // (2 * experts)
    slots = -(-cap // 16) * 16
    hidden = gate_weight.shape[2]
    held = experts * cap

    def v(*shape, dtype=BF16):
        return pltpu.VMEM(shape, dtype)

    scratch = [
        v(nz, 2 * rows_a, LANES), v(nz, 2 * rows_a, LANES), v(rows_a, LANES), v(1, nz * 2 * rows_a, dtype=F32),
        v(rows_a, 2 * LANES, dtype=F32), v(rows_a, LANES, dtype=F32),
        v(LANES, width), v(ny, nx, rows_a, LANES), v(rows_a, LANES),
        v(rows_m, width), v(width, hidden), v(width, hidden), v(hidden, width),
        v(experts, slots, LANES), v(experts, slots, LANES), v(ny, nx, held, LANES), v(ny, nx, held, LANES),
        v(experts, slots, LANES), v(experts, slots, LANES), v(LANES, -(-rows_m // LANES) * LANES, dtype=F32),
        pltpu.SemaphoreType.DMA((SEM_LIMIT,)),
        pltpu.SemaphoreType.DMA((2 * nz,)), pltpu.SemaphoreType.DMA((2 * nz,)),
        pltpu.SemaphoreType.DMA((2 * nz,)), pltpu.SemaphoreType.DMA((2 * nz,)),
        pltpu.SemaphoreType.DMA((9,)),
        *sum_buffers(nx, ny, rows_a),
        *sum_buffers(nx, ny, held),
    ]
    hbm = pl.BlockSpec(memory_space=pl.ANY)
    vm = pl.BlockSpec(memory_space=pltpu.VMEM)
    return pl.pallas_call(
        functools.partial(kernel, (nz, nx, ny, cap, slots, moe_at)),
        out_shape=(
            pltpu.VMEM((rows_a, LANES), BF16),
            pltpu.VMEM((rows_m, LANES), BF16),
        ),
        in_specs=[hbm] * 6 + [vm] * 4 + [hbm] * 3,
        out_specs=(vm, vm),
        scratch_shapes=scratch,
        compiler_params=pltpu.CompilerParams(
            collective_id=0, has_side_effects=True, vmem_limit_bytes=60 * 1024 * 1024
        ),
        name="step",
    )(
        queries, keys, values, log_gate_sums.T, mixer_weight, moe_rows, route_ids.T,
        group_gate.reshape(1, -1), inner_gate.T, norm_gain.reshape(1, -1), gate_weight[0], up_weight[0], down_weight[0],
    )


MOE_AT = (6, 8, 9, 12, 16, 17, 18, 20, 24, 28, 32, 100, 103)


def plane_of(tp):
    side = 1
    while side * side < tp:
        side *= 2
    return side, tp // side


def solution(mesh, plane=None, moe_at=MOE_AT):
    nx, ny = plane or plane_of(mesh.shape["tp"])
    sizes = (mesh.shape["ep"] // 2, nx, ny)
    return jax.shard_map(
        functools.partial(body, sizes, moe_at),
        mesh=mesh,
        in_specs=(
            P("ep", "tp"),
            P("ep", "tp"),
            P("ep", "tp"),
            P(None, "tp"),
            P("tp", None),
            P("ep", None),
            P("ep", None),
            P("ep"),
            P("ep", None),
            P(),
            P("ep", None, "tp"),
            P("ep", None, "tp"),
            P("ep", "tp", None),
        ),
        out_specs=(P("ep", "tp"), P("ep", "tp")),
        check_vma=False,
    )
```
